128 devices in a mesh: sp: 32 (over z, y, core), tp: 4 (over x).
Axes of the slice: x: 4, y: 4, z: 4, core: 2. Of those that a mesh axis runs over, the one named last changes fastest.
Arguments:
- residual: bfloat16 [8192, 2048], P('sp'), may hold values from -6 to 6
- queries: bfloat16 [8192, 8, 2, 128], P('sp', 'tp'), may hold values from -100 to 100
- key_rows: bfloat16 [8192, 8, 2, 128], P('sp', 'tp'), may hold values from -6 to 6
- values: bfloat16 [8192, 8, 256], P('sp', 'tp'), may hold values from -6 to 6
- lambda_head: float32 [8], P('tp'), may hold values from 0.3 to 0.8
- sub_gain: float32 [256], replicated, may hold values from 0.1 to 1.9
- w_out: bfloat16 [2048, 2048], P('tp'), may hold values from -0.125 to 0.125
- norm_gain: float32 [2048], replicated, may hold values from 0.1 to 1.9
- w_gate: bfloat16 [2048, 5632], P('sp', 'tp'), may hold values from -0.125 to 0.125
- w_up: bfloat16 [2048, 5632], P('sp', 'tp'), may hold values from -0.125 to 0.125
- conv_gate: float32 [3, 5632], P(None, 'tp'), may hold values from -3 to 3
- conv_up: float32 [3, 5632], P(None, 'tp'), may hold values from -3 to 3
- w_down: bfloat16 [5632, 2048], P('tp'), may hold values from -0.078125 to 0.078125
Outputs:
- layer_out: bfloat16 [8192, 2048], P(('sp', 'tp'))
The draws below stay inside these ranges and needn't reach their ends.
All inputs are finite; a program needn't handle non-finite values.
Results may differ from the reference program's by a relative error of at most 0.017.
Values may be sent and summed in bfloat16 or wider, within the bound.
No kernel may reach another device: no remote copies, remote signals or barrier semaphores. Data moves between devices by JAX's collectives and lax.ppermute only.
A program may use at most 192 MiB of HBM per device.

```python
import math
import jax
import jax.numpy as jnp
from jax import lax

D = 2048
HEADS = 8
DH = 128
DV = 256
FF = 5632
TOKENS = 8192


def query_key_pair(key):
    shape = (TOKENS, HEADS, 2, DH)
    keys_drawn = jnp.clip(1.3 * jax.random.normal(jax.random.fold_in(key, 12), shape, jnp.float32), -6.0, 6.0)
    queries_drawn = jnp.clip(1.3 * jax.random.normal(jax.random.fold_in(key, 11), shape, jnp.float32), -6.0, 6.0)
    return (queries_drawn, keys_drawn)


def draw_queries(key, part):
    return query_key_pair(key)[0].astype(jnp.bfloat16)


def draw_key_rows(key, part):
    return query_key_pair(key)[1].astype(jnp.bfloat16)


def block_scale(stream_key, extent, pieces, low, largest):
    def one(dim, shards_of):
        steps = jax.random.uniform(jax.random.fold_in(jax.random.fold_in(stream_key, 6), dim), (shards_of,), jnp.float32, low / len(pieces), largest / len(pieces))
        return jnp.repeat(jnp.exp(steps), extent[dim] // shards_of).reshape((-1,) + (1,) * (len(extent) - dim - 1))

    level = one(*pieces[0])
    for cut in pieces[1:]:
        level = level * one(*cut)
    return level


def normal_values(stream_key, dims, width, reach, split=(), held_as=jnp.bfloat16):
    result = width * jax.random.normal(stream_key, dims, jnp.float32)
    if split:
        result = result * block_scale(stream_key, dims, split, -0.22, 0.18)
    return jnp.clip(result, -reach, reach).astype(held_as)


def setup_inputs(seed: int = 0) -> dict:
    seeds = jax.random.split(jax.random.key(seed), 14)
    return {
        "residual": normal_values(seeds[0], (TOKENS, D), 1.0, 6.0, ((0, 32),)),
        "queries": draw_queries(jax.random.fold_in(seeds[13], 71), 0),
        "key_rows": draw_key_rows(jax.random.fold_in(seeds[13], 71), 0),
        "values": normal_values(seeds[3], (TOKENS, HEADS, DV), 1.0, 6.0, ((0, 32), (1, 4))),
        "lambda_head": jnp.clip(0.3 + 0.5 * jax.random.uniform(seeds[4], (HEADS,), jnp.float32) ** block_scale(seeds[4], (HEADS,), ((0, 4),), -0.2, 0.2), 0.3, 0.8),
        "sub_gain": jnp.clip(1.0 + 0.18 * jax.random.normal(seeds[5], (DV,), jnp.float32), 0.1, 1.9),
        "w_out": normal_values(seeds[6], (HEADS * DV, D), (HEADS * DV) ** -0.5, 0.125, ((0, 4),)),
        "norm_gain": jnp.clip(1.0 + 0.18 * jax.random.normal(seeds[7], (D,), jnp.float32), 0.1, 1.9),
        "w_gate": normal_values(seeds[8], (D, FF), D ** -0.5, 0.125, ((0, 32), (1, 4))),
        "w_up": normal_values(seeds[9], (D, FF), D ** -0.5, 0.125, ((0, 32), (1, 4))),
        "conv_gate": normal_values(seeds[10], (3, FF), 0.577, 3.0, ((1, 4),), jnp.float32),
        "conv_up": normal_values(seeds[11], (3, FF), 0.577, 3.0, ((1, 4),), jnp.float32),
        "w_down": normal_values(seeds[12], (FF, D), FF ** -0.5, 0.078125, ((0, 4),)),
    }


epsilon = 1e-06
lambda_init = 0.8 - 0.6 * math.exp(-0.3)

def causal_mix(rows_in, taps):
    padded_rows = jnp.concatenate([jnp.zeros((2, rows_in.shape[1]), jnp.float32), rows_in.astype(jnp.float32)], 0)
    return taps[0] * padded_rows[:-2] + taps[1] * padded_rows[1:-1] + taps[2] * padded_rows[2:]

def reference(residual, queries, key_rows, values, lambda_head, sub_gain, w_out, norm_gain, w_gate, w_up, conv_gate, conv_up, w_down):
    query_block = math.gcd(TOKENS, 256)
    score_scale = 1.0 / math.sqrt(DH)
    key_pos = jnp.arange(TOKENS, dtype=jnp.int32)
    keys_wide = key_rows.astype(jnp.float32)
    values_wide = values.astype(jnp.float32)

    def attend(block_start):
        query_part = lax.dynamic_slice_in_dim(queries, block_start, query_block, 0).astype(jnp.float32)
        scores = jnp.einsum('qhcd,khcd->hcqk', query_part, keys_wide) * score_scale
        query_pos = block_start + jnp.arange(query_block, dtype=jnp.int32)
        causal_mask = key_pos[None, :] <= query_pos[:, None]
        scores = jnp.where(causal_mask, scores, -1e+30)
        run_max = lax.optimization_barrier(jnp.max(scores, axis=-1, keepdims=True))
        weights = jnp.where(causal_mask, jnp.exp(scores - run_max), 0.0)
        run_sum = lax.optimization_barrier(jnp.sum(weights, axis=-1))
        rounded = lax.optimization_barrier(weights.astype(jnp.bfloat16)).astype(jnp.float32)
        summed = jnp.einsum('hcqk,khe->hcqe', rounded, values_wide)
        blended = summed / run_sum[..., None]
        return blended[:, 0] - lambda_head[:, None, None] * blended[:, 1]
    starts = (jnp.arange(TOKENS // query_block, dtype=jnp.int32) * query_block).astype(jnp.int32)
    attended = lax.map(attend, starts)
    attended = jnp.transpose(attended, (0, 2, 1, 3)).reshape(TOKENS, HEADS, DV)
    mean_square = lax.optimization_barrier(jnp.mean(attended * attended, axis=-1, keepdims=True))
    normed = attended * lax.rsqrt(mean_square + epsilon) * sub_gain * (1.0 - lambda_init)
    normed = normed.astype(jnp.bfloat16).reshape(TOKENS, HEADS * DV)
    middle = residual.astype(jnp.float32) + jnp.dot(normed, w_out, preferred_element_type=jnp.float32)
    row_square = lax.optimization_barrier(jnp.mean(middle * middle, axis=-1, keepdims=True))
    normed_rows = (middle * lax.rsqrt(row_square + epsilon) * norm_gain).astype(jnp.bfloat16)
    gate_pre = jnp.dot(normed_rows, w_gate, preferred_element_type=jnp.float32).astype(jnp.bfloat16)
    up_pre = jnp.dot(normed_rows, w_up, preferred_element_type=jnp.float32).astype(jnp.bfloat16)
    gate_mixed = causal_mix(gate_pre, conv_gate)
    up_mixed = causal_mix(up_pre, conv_up)
    hidden = (jax.nn.silu(gate_mixed) * up_mixed).astype(jnp.bfloat16)
    lowered = jnp.dot(hidden, w_down, preferred_element_type=jnp.float32)
    return (middle + lowered).astype(jnp.bfloat16)
```

```python
import math

import jax
import jax.numpy as jnp
from jax import lax
from jax.experimental import pallas as pl
from jax.experimental.pallas import tpu as pltpu
from jax.sharding import Mesh, PartitionSpec as P

EPS = 1e-06
LAMBDA_INIT = 0.8 - 0.6 * math.exp(-0.3)
LOG2E = math.log2(math.e)
NEG = -1e30
F32 = jnp.float32
BF16 = jnp.bfloat16
SHIFTS = (1, 3, 2)
VMEM = pltpu.VMEM


def vspec():
    return pl.BlockSpec(memory_space=pltpu.VMEM)


def moved(x, axis, by):
    n = 4
    return lax.ppermute(x, axis, [(i, (i + by) % n) for i in range(n)])


def swapped(x):
    return lax.ppermute(x, "c", [(0, 1), (1, 0)])


def attend(qs, kv_same, kv_other, heads, dh, dv):
    rows = qs[0].shape[0]
    maps = heads * 2
    kcols = maps * dh
    scale = LOG2E / math.sqrt(dh)

    def body(*refs):
        q_in, same_in, other_in = refs[0:4], refs[4:8], refs[8:12]
        o_ref, st_ref = refs[12:14]
        q_scr, kv_scr, m_scr, l_scr, acc_scr, sem = refs[14:]
        z, y, c = lax.axis_index("z"), lax.axis_index("y"), lax.axis_index("c")
        slot = pl.program_id(0)

        def copies():
            out = []
            for d in range(4):
                out.append(pltpu.make_async_copy(q_in[d], q_scr.at[d], sem.at[d]))
            for d in range(4):
                at = lax.rem(z - d + 4, 4)
                out.append(pltpu.make_async_copy(same_in[d], kv_scr.at[at, c], sem.at[4 + d]))
                out.append(pltpu.make_async_copy(other_in[d], kv_scr.at[at, 1 - c], sem.at[8 + d]))
            return out

        @pl.when(slot == 0)
        def _():
            made = copies()
            for x in made:
                x.start()
            for x in made:
                x.wait()

        m_scr[...] = jnp.full_like(m_scr, NEG)
        l_scr[...] = jnp.zeros_like(l_scr)
        acc_scr[...] = jnp.zeros_like(acc_scr)

        def step(j, masked):
            keep = None
            if masked:
                col = lax.broadcasted_iota(jnp.int32, (rows, 2 * rows), 1)
                row = lax.broadcasted_iota(jnp.int32, (rows, 2 * rows), 0)
                keep = col <= row + c * rows
            for i in range(maps):
                q = q_scr[slot, :, i * dh : (i + 1) * dh]
                k = kv_scr[j, :, :, i * dh : (i + 1) * dh].reshape(2 * rows, dh)
                h = i // 2
                v = kv_scr[j, :, :, kcols + h * dv : kcols + (h + 1) * dv].reshape(2 * rows, dv)
                s = lax.dot_general(q, k, (((1,), (1,)), ((), ())), preferred_element_type=F32)
                if masked:
                    s = jnp.where(keep, s, NEG)
                m_old = m_scr[i, :, 0:1]
                m_new = jnp.maximum(m_old, jnp.max(s, axis=1, keepdims=True))
                e = jnp.exp2((s - m_new) * scale)
                alpha = jnp.exp2((m_old - m_new) * scale)
                l_scr[i] = l_scr[i] * alpha + jnp.sum(e, axis=1, keepdims=True)
                acc_scr[i] = acc_scr[i] * alpha + jnp.dot(e.astype(BF16), v, preferred_element_type=F32)
                m_scr[i] = jnp.broadcast_to(m_new, m_scr.shape[1:])

        yq = lax.rem(y - slot + 4, 4)
        full = z + (yq > y).astype(jnp.int32)

        @pl.loop(0, full)
        def _(j):
            step(j, False)

        @pl.when(slot == 0)
        def _():
            step(z, True)

        lane = lax.broadcasted_iota(jnp.int32, (rows, 128), 1)
        st = jnp.zeros((rows, 128), F32)
        for i in range(maps):
            o_ref[:, i * dv : (i + 1) * dv] = acc_scr[i]
            st = jnp.where(lane == i, m_scr[i], st)
            st = jnp.where(lane == maps + i, l_scr[i], st)
        st_ref[...] = jnp.transpose(st)[0 : 2 * maps, :]

    any_spec = pl.BlockSpec(memory_space=pl.ANY)
    return pl.pallas_call(
        body,
        grid=(4,),
        out_shape=(
            jax.ShapeDtypeStruct((4 * rows, maps * dv), F32),
            jax.ShapeDtypeStruct((2 * maps, 4 * rows), F32),
        ),
        in_specs=[any_spec] * 12,
        out_specs=(
            pl.BlockSpec((rows, maps * dv), lambda s: (s, 0)),
            pl.BlockSpec((2 * maps, rows), lambda s: (0, s)),
        ),
        scratch_shapes=[
            VMEM((4, rows, kcols), BF16),
            VMEM((4, 2, rows, kcols + heads * dv), BF16),
            VMEM((maps, rows, 128), F32),
            VMEM((maps, rows, 128), F32),
            VMEM((maps, rows, dv), F32),
            pltpu.SemaphoreType.DMA((12,)),
        ],
        name="attend",
    )(*qs, *kv_same, *kv_other)


def blend(o, stats, lam, heads, dh, dv):
    rows = o.shape[0] // 4
    maps = heads * 2
    scale = LOG2E / math.sqrt(dh)

    def body(lam_ref, o_ref, s0, s1, s2, s3, a0, a1, a2, a3):
        st = (s0, s1, s2, s3)
        for d, out in enumerate((a0, a1, a2, a3)):
            ms, ls = [], []
            for e in range(4):
                at = ((d - e) % 4) * rows
                ms.append(st[e][0:maps, at : at + rows])
                ls.append(st[e][maps : 2 * maps, at : at + rows])
            top = jnp.maximum(jnp.maximum(ms[0], ms[1]), jnp.maximum(ms[2], ms[3]))
            total = sum(l * jnp.exp2((m - top) * scale) for m, l in zip(ms, ls))
            coef = jnp.exp2((ms[0] - top) * scale) / total
            wide = jnp.transpose(jnp.concatenate([coef, jnp.zeros((128 - maps, rows), F32)], 0))
            for h in range(heads):
                i = 2 * h
                c0 = wide[:, i : i + 1]
                c1 = wide[:, i + 1 : i + 2] * lam_ref[h]
                blk = pl.ds(d * rows, rows)
                a = o_ref[blk, i * dv : (i + 1) * dv] * c0 - o_ref[blk, (i + 1) * dv : (i + 2) * dv] * c1
                out[:, h * dv : (h + 1) * dv] = a.astype(out.dtype)

    shapes = [jax.ShapeDtypeStruct((rows, heads * dv), F32 if d == 0 else BF16) for d in range(4)]
    return pl.pallas_call(
        body,
        out_shape=shapes,
        in_specs=[pl.BlockSpec(memory_space=pltpu.SMEM)] + [vspec()] * 5,
        out_specs=[vspec()] * 4,
        name="blend",
    )(lam, o, *stats)


def head_norm(parts, gain, heads, dv):
    rows = parts[0].shape[0]

    def body(p0, p1, p2, p3, g, out):
        for h in range(heads):
            cols = slice(h * dv, (h + 1) * dv)
            a = p0[:, cols] + p1[:, cols].astype(F32) + p2[:, cols].astype(F32) + p3[:, cols].astype(F32)
            ms = jnp.mean(a * a, axis=1, keepdims=True)
            out[h] = (a * lax.rsqrt(ms + EPS) * g[...] * (1.0 - LAMBDA_INIT)).astype(BF16)

    return pl.pallas_call(
        body,
        out_shape=jax.ShapeDtypeStruct((heads, rows, dv), BF16),
        in_specs=[vspec()] * 5,
        out_specs=vspec(),
        name="head_norm",
    )(*parts, gain.reshape(1, dv))


def project(ns, w_own, w_same, w_other, residual, norm_gain):
    heads, rows, dv = ns[0].shape
    width = residual.shape[1]
    tile = 512
    steps = width // tile

    def body(n0, n1, n2, n3, wo, ws1, ws2, ws3, wp1, wp2, wp3, res, gain, hn_ref, own_ref, mid):
        c, t = lax.axis_index("c"), lax.axis_index("tp")
        j = pl.program_id(0)
        acc = res[...].astype(F32)
        for h in range(heads):
            acc += jnp.dot(n0[h], wo[h], preferred_element_type=F32)
        for n, ws, wp in ((n1, ws1, wp1), (n2, ws2, wp2), (n3, ws3, wp3)):
            acc += jnp.dot(n[c], ws[...], preferred_element_type=F32)
            acc += jnp.dot(n[1 - c], wp[...], preferred_element_type=F32)
        mid[j] = acc

        @pl.when(j == steps - 1)
        def _():
            sq = sum(jnp.sum(mid[i] * mid[i], axis=1, keepdims=True) for i in range(steps))
            r = lax.rsqrt(sq / width + EPS)
            own = rows // 4
            at = pl.ds(pl.multiple_of(t * own, own), own)
            for i in range(steps):
                cols = slice(i * tile, (i + 1) * tile)
                hn_ref[:, cols] = (mid[i] * r * gain[:, cols]).astype(BF16)
                own_ref[:, cols] = mid[i, at, :]

    whole3 = pl.BlockSpec((heads, rows, dv), lambda j: (0, 0, 0))
    wcol = pl.BlockSpec((dv, tile), lambda j: (0, j))
    return pl.pallas_call(
        body,
        grid=(steps,),
        out_shape=(
            jax.ShapeDtypeStruct((rows, width), BF16),
            jax.ShapeDtypeStruct((rows // 4, width), F32),
        ),
        in_specs=[whole3] * 4
        + [pl.BlockSpec((heads, dv, tile), lambda j: (0, 0, j))]
        + [wcol] * 6
        + [pl.BlockSpec((rows, tile), lambda j: (0, j)), pl.BlockSpec((1, width), lambda j: (0, 0))],
        out_specs=(
            pl.BlockSpec((rows, width), lambda j: (0, 0)),
            pl.BlockSpec((rows // 4, width), lambda j: (0, 0)),
        ),
        scratch_shapes=[VMEM((steps, rows, tile), F32)],
        name="project",
    )(*ns, w_own, *w_same, *w_other, residual, norm_gain.reshape(1, width))


def gate_up(hn, w):
    rows, width = hn.shape
    cols = w.shape[1]
    tile = 256
    tail = 16

    def body(x, w_ref, out, tail_ref):
        r = jnp.dot(x[...], w_ref[...], preferred_element_type=F32).astype(BF16)
        out[...] = r
        tail_ref[...] = r[rows - tail :, :]

    return pl.pallas_call(
        body,
        grid=(cols // tile,),
        out_shape=(jax.ShapeDtypeStruct((rows, cols), BF16), jax.ShapeDtypeStruct((tail, cols), BF16)),
        in_specs=[pl.BlockSpec((rows, width), lambda j: (0, 0)), pl.BlockSpec((width, tile), lambda j: (0, j))],
        out_specs=(pl.BlockSpec((rows, tile), lambda j: (0, j)), pl.BlockSpec((tail, tile), lambda j: (0, j))),
        name="gate_up",
    )(hn, w)


def down(gu, prior, conv_gate, conv_up, w_down):
    rows, cols = gu.shape
    hid = cols // 2
    width = w_down.shape[1]
    tile = 512
    tail = prior.shape[0]
    own = rows // 4

    def body(gu_ref, pr, cg, cu, w_ref, o0, o1, o2, o3, hidden, low):
        t = lax.axis_index("tp")

        @pl.when(pl.program_id(0) == 0)
        def _():
            step = 128
            for at in range(0, hid, step):
                mixed = []
                for taps, base in ((cg, 0), (cu, hid)):
                    cs = slice(base + at, base + at + step)
                    x = gu_ref[:, cs].astype(F32)
                    p = pr[:, cs].astype(F32)
                    ts = slice(at, at + step)
                    row = lax.broadcasted_iota(jnp.int32, x.shape, 0)
                    one = jnp.where(row == 0, p[tail - 1 : tail], pltpu.roll(x, 1, 0))
                    two = pltpu.roll(x, 2, 0)
                    two = jnp.where(row == 0, p[tail - 2 : tail - 1], two)
                    two = jnp.where(row == 1, p[tail - 1 : tail], two)
                    mixed.append(taps[0:1, ts] * two + taps[1:2, ts] * one + taps[2:3, ts] * x)
                g, u = mixed
                hidden[:, at : at + step] = (g / (1.0 + jnp.exp(-g)) * u).astype(BF16)

        low[...] = jnp.dot(hidden[...], w_ref[...], preferred_element_type=F32)
        for d, out in enumerate((o0, o1, o2, o3)):
            at = lax.rem(t + d, 4) * own
            out[...] = low[pl.ds(pl.multiple_of(at, own), own), :].astype(out.dtype)

    return pl.pallas_call(
        body,
        grid=(width // tile,),
        out_shape=[jax.ShapeDtypeStruct((own, width), F32 if d == 0 else BF16) for d in range(4)],
        in_specs=[
            pl.BlockSpec((rows, cols), lambda j: (0, 0)),
            pl.BlockSpec((tail, cols), lambda j: (0, 0)),
            pl.BlockSpec((3, hid), lambda j: (0, 0)),
            pl.BlockSpec((3, hid), lambda j: (0, 0)),
            pl.BlockSpec((hid, tile), lambda j: (0, j)),
        ],
        out_specs=[pl.BlockSpec((own, tile), lambda j: (0, j))] * 4,
        scratch_shapes=[VMEM((rows, hid), BF16), VMEM((rows, tile), F32)],
        name="down",
    )(gu, prior, conv_gate, conv_up, w_down)


def local(residual, queries, key_rows, values, lambda_head, sub_gain, w_out, norm_gain, w_gate, w_up, conv_gate, conv_up, w_down):
    rows, heads, _, dh = queries.shape
    dv = values.shape[2]
    c = lax.axis_index("c")
    q = queries.reshape(rows, heads * 2 * dh)
    kv = jnp.concatenate([key_rows.reshape(rows, heads * 2 * dh), values.reshape(rows, heads * dv)], 1)
    w_pack = jnp.concatenate([w_gate, w_up], 1)
    w_full = lax.all_gather(w_pack, ("z", "y", "c"), axis=0, tiled=True)

    kv_same = {0: kv}
    qs = {0: q}
    for d in SHIFTS:
        kv_same[d] = moved(kv, "z", d)
        qs[d] = moved(q, "y", d)
    w_heads = w_out.reshape(heads, dv, w_out.shape[1])
    w_half = lax.dynamic_index_in_dim(w_heads, c, 0, keepdims=False)
    w_same = {d: moved(w_half, "tp", d) for d in SHIFTS}
    kv_other = {d: swapped(kv_same[d]) for d in range(4)}
    w_other = {d: swapped(w_same[d]) for d in SHIFTS}

    order = range(4)
    o, st = attend([qs[d] for d in order], [kv_same[d] for d in order], [kv_other[d] for d in order], heads, dh, dv)
    stats = {0: st}
    for d in SHIFTS:
        stats[d] = moved(st, "y", d)
    a = blend(o, [stats[d] for d in order], lambda_head, heads, dh, dv)
    parts = [a[0]] + [moved(a[d], "y", -d) for d in SHIFTS]
    n = head_norm(parts, sub_gain, heads, dv)
    ns = [n] + [moved(n, "tp", d) for d in (1, 2, 3)]
    hn, mid_own = project(ns, w_heads, [w_same[d] for d in (1, 2, 3)], [w_other[d] for d in (1, 2, 3)], residual, norm_gain)
    gu, tail = gate_up(hn, w_full)
    total = 32
    prior = lax.ppermute(tail, ("z", "y", "c"), [(i, i + 1) for i in range(total - 1)])
    low = down(gu, prior, conv_gate, conv_up, w_down)
    out = mid_own + low[0]
    for d in SHIFTS:
        out = out + moved(low[d], "tp", d).astype(F32)
    return out.astype(BF16)


def solution(mesh):
    split = Mesh(mesh.devices.reshape(4, 4, 2, 4), ("z", "y", "c", "tp"))
    sp = ("z", "y", "c")
    placed = (
        P(sp, None),
        P(sp, "tp", None, None),
        P(sp, "tp", None, None),
        P(sp, "tp", None),
        P("tp"),
        P(),
        P("tp", None),
        P(),
        P(sp, "tp"),
        P(sp, "tp"),
        P(None, "tp"),
        P(None, "tp"),
        P("tp", None),
    )
    return jax.shard_map(local, mesh=split, in_specs=placed, out_specs=P((*sp, "tp"), None), check_vma=False)
```
